512 devices in a mesh: sp: 64 (over z, y), tp: 8 (over x, core).
Axes of the slice: x: 4, y: 8, z: 8, core: 2. Of those that a mesh axis runs over, the one named last changes fastest.
Arguments:
- queries: bfloat16 [32768, 2048], P('sp', 'tp'), may hold values from -14 to 14
- key_states: bfloat16 [32768, 512], P('sp', 'tp'), may hold values from -14 to 14
- value_states: bfloat16 [32768, 512], P('sp', 'tp'), may hold values from -6 to 6
- sink_logits: float32 [32], P('tp'), may hold values from 0 to 5
- out_weight: bfloat16 [2048, 2048], P('tp'), may hold values from -0.125 to 0.125
- residual: bfloat16 [32768, 2048], P(('sp', 'tp')), may hold values from -6 to 6
- gain_attn: float32 [2048], replicated, may hold values from 0.1 to 1.9
- gain_before: float32 [2048], replicated, may hold values from 0.1 to 1.9
- gain_after: float32 [2048], replicated, may hold values from 0.1 to 1.9
- gate_weight: bfloat16 [2048, 5632], P('sp', 'tp'), may hold values from -0.125 to 0.125
- value_weight: bfloat16 [2048, 5632], P('sp', 'tp'), may hold values from -0.125 to 0.125
- gate_taps: float32 [3, 5632], P(None, 'tp'), may hold values from -3 to 3
- value_taps: float32 [3, 5632], P(None, 'tp'), may hold values from -3 to 3
- down_weight: bfloat16 [5632, 2048], P('tp', 'sp'), may hold values from -0.078125 to 0.078125
Outputs:
- layer_out: bfloat16 [32768, 2048], P(('sp', 'tp'))
The draws below stay inside these ranges and needn't reach their ends.
All inputs are finite; a program needn't handle non-finite values.
Results may differ from the reference program's by a relative error of at most 0.018.
Values may be sent and summed in bfloat16 or wider, within the bound.
A program may use at most 64 MiB of HBM per device.

```python
import jax
import jax.numpy as jnp
from jax import lax

D = 2048
HQ = 32
KV = 8
HD = 64
FF = 5632
WINDOW = 128
CONVK = 3
TOKENS = 32768
N_TP = 8


def drawn_keys(key):
    base = jax.random.truncated_normal(jax.random.fold_in(key, 11), -2.5, 2.5, (TOKENS, KV * HD), jnp.float32)
    return base


def draw_key_states(key, part):
    base = drawn_keys(key)
    return base.astype(jnp.bfloat16)


def draw_queries(key, part):
    own = jax.random.truncated_normal(jax.random.fold_in(key, 21), -2.5, 2.5, (TOKENS, HQ * HD), jnp.float32)
    return own.astype(jnp.bfloat16)


def block_scale(key, shape, cuts, smallest, high):
    loudness, own = 1.0, jax.random.fold_in(key, 6)
    for axis_at, blocks in cuts:
        steps = jnp.exp(jax.random.uniform(jax.random.fold_in(own, axis_at), (blocks,), jnp.float32, smallest / len(cuts), high / len(cuts)))
        loudness = loudness * jnp.repeat(steps, shape[axis_at] // blocks).reshape([-1 if axis == axis_at else 1 for axis in range(len(shape))])
    return loudness


def scatter_about(rng, extent, scale, most, shards=(), kind=jnp.bfloat16):
    loudness = block_scale(rng, extent, shards, -0.22, 0.18) if shards else 1.0
    drawn = jax.random.normal(rng, extent, jnp.float32) * scale * loudness
    return jnp.minimum(jnp.maximum(drawn, -most), most).astype(kind)


def setup_inputs(seed: int = 0) -> dict:
    arg_keys = jax.random.split(jax.random.key(seed), 15)
    return {
        "queries": draw_queries(jax.random.fold_in(arg_keys[14], 71), 0),
        "key_states": draw_key_states(jax.random.fold_in(arg_keys[14], 71), 0),
        "value_states": scatter_about(arg_keys[2], (TOKENS, KV * HD), 1.0, 6.0, ((0, 64), (1, 8))),
        "sink_logits": jnp.clip(5.0 * jax.random.uniform(arg_keys[3], (HQ,), jnp.float32) ** block_scale(arg_keys[3], (HQ,), ((0, 8),), -0.2, 0.2), 0.0, 5.0),
        "out_weight": scatter_about(arg_keys[4], (HQ * HD, D), (HQ * HD) ** -0.5, 0.125, ((0, 8),)),
        "residual": scatter_about(arg_keys[5], (TOKENS, D), 1.0, 6.0, ((0, 512),)),
        "gain_attn": jnp.clip(1.0 + 0.18 * jax.random.normal(arg_keys[6], (D,), jnp.float32), 0.1, 1.9),
        "gain_before": jnp.clip(1.0 + 0.18 * jax.random.normal(arg_keys[7], (D,), jnp.float32), 0.1, 1.9),
        "gain_after": jnp.clip(1.0 + 0.18 * jax.random.normal(arg_keys[8], (D,), jnp.float32), 0.1, 1.9),
        "gate_weight": scatter_about(arg_keys[9], (D, FF), D ** -0.5, 0.125, ((0, 64), (1, 8))),
        "value_weight": scatter_about(arg_keys[10], (D, FF), D ** -0.5, 0.125, ((0, 64), (1, 8))),
        "gate_taps": scatter_about(arg_keys[11], (CONVK, FF), 0.577, 3.0, ((1, 8),), jnp.float32),
        "value_taps": scatter_about(arg_keys[12], (CONVK, FF), 0.577, 3.0, ((1, 8),), jnp.float32),
        "down_weight": scatter_about(arg_keys[13], (FF, D), FF ** -0.5, 0.078125, ((0, 8), (1, 64))),
    }


NEG_FILL = -1e+30

def rms_scale(matrix):
    return matrix * lax.rsqrt(lax.optimization_barrier(jnp.mean(matrix * matrix, axis=-1, keepdims=True)) + 1e-06)

def attention(queries, key_states, value_states, sink_logits):
    length = queries.shape[0]
    blocks = length // WINDOW
    grouping = HQ // KV
    zeros_rows = jnp.zeros((WINDOW, KV * HD), jnp.bfloat16)
    keys_ext = jnp.concatenate([zeros_rows, key_states], axis=0).reshape(blocks + 1, WINDOW, KV, HD)
    values_ext = jnp.concatenate([zeros_rows, value_states], axis=0).reshape(blocks + 1, WINDOW, KV, HD)
    key_blocks = jnp.concatenate([keys_ext[:-1], keys_ext[1:]], axis=1)
    value_blocks = jnp.concatenate([values_ext[:-1], values_ext[1:]], axis=1)
    query_blocks = queries.reshape(blocks, WINDOW, KV, grouping, HD)
    qpos = jnp.arange(length, dtype=jnp.int32).reshape(blocks, WINDOW)
    kpos = jnp.concatenate([qpos - WINDOW, qpos], axis=1)
    visible = (kpos[:, None, :] <= qpos[:, :, None]) & (qpos[:, :, None] - kpos[:, None, :] < WINDOW) & (kpos[:, None, :] >= 0)
    sinks_all = sink_logits.reshape(KV, grouping)

    def one_head(inputs):
        query_part, key_part, value_part, sink_part = inputs
        scores = jnp.einsum('nqgd,nkd->ngqk', query_part.astype(jnp.float32), key_part.astype(jnp.float32)) * HD ** (-0.5)
        scores = jnp.where(visible[:, None], scores, NEG_FILL)
        sink_col = sink_part[None, :, None]
        top = jnp.maximum(lax.optimization_barrier(jnp.max(scores, axis=-1)), sink_col)
        expo = jnp.exp(scores - top[..., None])
        total = lax.optimization_barrier(jnp.sum(expo, axis=-1)) + jnp.exp(sink_col - top)
        probs = (expo / total[..., None]).astype(jnp.bfloat16)
        result = jnp.einsum('ngqk,nkd->nqgd', probs.astype(jnp.float32), value_part.astype(jnp.float32))
        return result.astype(jnp.bfloat16)
    heads_out = lax.map(one_head, (jnp.moveaxis(query_blocks, 2, 0), jnp.moveaxis(key_blocks, 2, 0), jnp.moveaxis(value_blocks, 2, 0), sinks_all))
    return jnp.moveaxis(heads_out, 0, 2).reshape(length, HQ * HD)

def grouped_sum(left, right):
    width = left.shape[1] // N_TP
    total = jnp.zeros((left.shape[0], right.shape[1]), jnp.float32)
    for group_index in range(N_TP):
        part = jnp.dot(left[:, group_index * width:(group_index + 1) * width], right[group_index * width:(group_index + 1) * width], preferred_element_type=jnp.float32)
        total = total + part.astype(jnp.bfloat16).astype(jnp.float32)
    return total

def causal_taps(upward, kernel):
    length = upward.shape[0]
    padded = jnp.concatenate([jnp.zeros((CONVK - 1, upward.shape[1]), jnp.bfloat16), upward], axis=0).astype(jnp.float32)
    result = jnp.zeros((length, upward.shape[1]), jnp.float32)
    for tap_index in range(CONVK):
        result = result + kernel[tap_index][None, :] * padded[tap_index:tap_index + length]
    return result

def reference(queries, key_states, value_states, sink_logits, out_weight, residual, gain_attn, gain_before, gain_after, gate_weight, value_weight, gate_taps, value_taps, down_weight):
    attended = attention(queries, key_states, value_states, sink_logits)
    attn_proj = grouped_sum(attended, out_weight)
    middle = residual.astype(jnp.float32) + rms_scale(attn_proj) * gain_attn
    normed = (rms_scale(middle) * gain_before).astype(jnp.bfloat16)
    gate_up = jnp.dot(normed, gate_weight, preferred_element_type=jnp.float32).astype(jnp.bfloat16)
    value_up = jnp.dot(normed, value_weight, preferred_element_type=jnp.float32).astype(jnp.bfloat16)
    gate_conv = causal_taps(gate_up, gate_taps)
    value_conv = causal_taps(value_up, value_taps)
    hidden = (jax.nn.silu(gate_conv) * value_conv).astype(jnp.bfloat16)
    down = grouped_sum(hidden, down_weight)
    return (middle + rms_scale(down) * gain_after).astype(jnp.bfloat16)
```

```python
import jax
import jax.numpy as jnp
from jax import lax
from jax.experimental import pallas as pl
from jax.experimental.pallas import tpu as pltpu
from jax.sharding import PartitionSpec as P

HD = 64
WINDOW = 128
NEG_FILL = -1e30
MESH = pl.DeviceIdType.MESH
F32 = jnp.float32
BF16 = jnp.bfloat16
NT = (((1,), (1,)), ((), ()))


def rms_scale(matrix):
    return matrix * lax.rsqrt(jnp.mean(matrix * matrix, axis=-1, keepdims=True) + 1e-06)


def kernel(
    q_ref, kt_ref, vt_ref, sink_ref, ow_ref, res_ref, ga_ref, gb_ref, gc_ref,
    gw_ref, vw_ref, gt_ref, vt2_ref, dw_ref,
    out_ref,
    gv, dn, kvx, att, x_all, up, hid, mid,
    p_own, p_sib, r_sib, s_x, r_x,
    f_own, f_sib, g_sib, t_x, u_x,
    rp1, rp2, ssem, kv_sem, up_ss, up_rs,
    a_ss, a_rs, ax_ss, ax_rs, b_ss, b_rs, bx_ss, bx_rs, g_ss, g_rs,
):
    sp = lax.axis_index("sp")
    tp = lax.axis_index("tp")
    z, y = sp // 8, sp % 8
    x, c = tp // 2, tp % 2

    def at(zz, yy):
        return (zz % 8) * 8 + yy % 8

    def tp_at(xx, cc):
        return (xx % 4) * 2 + cc

    nxt, prv = ((sp + 1) % 64, tp), ((sp + 63) % 64, tp)
    sib = (sp, tp_at(x, 1 - c))
    xp, xm = (sp, tp_at(x + 1, c)), (sp, tp_at(x + 3, c))
    zn = ((at(z + 1, y), tp), (at(z + 7, y), tp))
    yn = ((at(z, y + 1), tp), (at(z, y + 7), tp))

    barrier = pltpu.get_barrier_semaphore()
    for dev in (nxt, prv, sib, xp, xm, *zn, *yn):
        pl.semaphore_signal(barrier, inc=1, device_id=dev, device_id_type=MESH)

    def remote(src, dst, ss, rs, dev):
        return pltpu.make_async_remote_copy(
            src_ref=src, dst_ref=dst, send_sem=ss, recv_sem=rs, device_id=dev, device_id_type=MESH
        )

    for h in range(2):
        rows = slice(16 * h, 16 * h + 16)
        for k in range(5):
            cols = slice(128 * k, 128 * k + 128)
            gv[z, y, h, :, 256 * k : 256 * k + 128] = gw_ref[rows, cols]
            gv[z, y, h, :, 256 * k + 128 : 256 * k + 256] = vw_ref[rows, cols]
            dn[z, y, h, :, cols] = dw_ref[rows, cols]
        gv[z, y, h, :, 1280:1408] = jnp.concatenate(
            [gw_ref[rows, 640:704].astype(F32), vw_ref[rows, 640:704].astype(F32)], axis=1
        ).astype(BF16)
        dn[z, y, h, :, 640:768] = jnp.concatenate(
            [dw_ref[rows, 640:704].astype(F32), jnp.zeros((16, 64), F32)], axis=1
        ).astype(BF16)
    kvx[0, :, 128:640] = kt_ref[...]
    kvx[1, :, 128:640] = vt_ref[...]

    pl.semaphore_wait(barrier, 9)

    def gather_steps(ps, buf):
        first = (y, z)
        second = (z, y)
        fdev = (yn, zn)
        sdev = (zn, yn)

        def item(h, f, s):
            f, s = f % 8, s % 8
            return buf.at[s, f, 0] if h == 0 else buf.at[f, s, 1]

        def batch(h, b, s):
            s = s % 8
            return buf.at[s, pl.ds(4 * b, 4), 0] if h == 0 else buf.at[pl.ds(4 * b, 4), s, 1]

        def send_first(h, d, k):
            f, s = first[h], second[h]
            ref = item(h, f + 9 - k if d == 0 else f + k - 1, s)
            remote(ref, ref, ssem.at[ps, h, d, 0], rp1.at[ps, h, d, k - 1], fdev[h][d]).start()

        def wait_first(h, d, k):
            f, s = first[h], second[h]
            ref = item(h, f + 8 - k if d == 0 else f + k, s)
            remote(ref, ref, ssem.at[ps, h, d, 0], rp1.at[ps, h, d, k - 1], fdev[h][d]).wait_recv()
            return f + 8 - k if d == 0 else f + k

        def send_own_group(h, f):
            f = f % 8
            ref = item(h, f, second[h])
            for d in range(2):
                remote(
                    ref, ref, ssem.at[ps, h, d, 1], rp2.at[ps, h, d, 0, f // 4], sdev[h][d]
                ).start()

        def group(h, d, k):
            return second[h] + 8 - k if d == 0 else second[h] + k

        def wait_second(h, d, k, b):
            ref = batch(h, b, group(h, d, k))
            remote(
                ref, ref, ssem.at[ps, h, d, 1], rp2.at[ps, h, d, k - 1, b], sdev[h][d]
            ).wait_recv()

        def forward(h, d, k, b):
            ref = batch(h, b, group(h, d, k))
            remote(
                ref, ref, ssem.at[ps, h, d, k + 1], rp2.at[ps, h, d, k, b], sdev[h][d]
            ).start()

        def step_own():
            for h in range(2):
                for d in range(2):
                    send_first(h, d, 1)
            for h in range(2):
                send_own_group(h, first[h])

        def step_first(k):
            def run():
                for d in range(2 if k < 4 else 1):
                    for h in range(2):
                        f = wait_first(h, d, k)
                        if k < (4 if d == 0 else 3):
                            send_first(h, d, k + 1)
                        send_own_group(h, f)

            return run

        def step_second(k, b):
            def run():
                for h in range(2):
                    for d in range(2):
                        wait_second(h, d, k, b)
                        if k < 3 or b == d:
                            forward(h, d, k, b)

            return run

        def step_last():
            for h in range(2):
                for d in range(2):
                    wait_second(h, d, 4, d)

        steps = [step_own] + [step_first(k) for k in range(1, 5)]
        steps += [step_second(k, b) for k in range(1, 4) for b in range(2)]
        steps.append(step_last)

        def finish():
            for h in range(2):
                for d in range(2):
                    for slot, ref in (
                        (0, buf.at[0, pl.ds(0, 4 - d), 0]),
                        (1, buf.at[0, :, 0]),
                        (2, buf.at[0, :, 0]),
                        (3, buf.at[0, :, 0]),
                        (4, buf.at[0, pl.ds(0, 4), 0]),
                    ):
                        remote(
                            ref, ref, ssem.at[ps, h, d, slot], rp1.at[ps, h, d, 0], sib
                        ).wait_send()

        return steps, finish

    wsteps, wfinish = gather_steps(0, gv)
    dsteps, dfinish = gather_steps(1, dn)

    order = (2, 1, 3, 0)

    def reducer(own, sendb, recvb, sx, rx, ss, rs, xss, xrs):
        dest = (xm, xp, xp, xp, xm, xm)

        def xcopy(j):
            return remote(sx.at[j], rx.at[j], xss.at[j], xrs.at[j], dest[j])

        def to_sib(i):
            return remote(sendb.at[i], recvb.at[i], ss.at[i], rs.at[i], sib)

        def total(i, half):
            rows = slice(32 * half, 32 * half + 32)
            return own[i, rows].astype(F32) + recvb[i, rows].astype(F32)

        def stage(i):
            to_sib(i).wait_recv()
            if i == 0:
                sx[0] = total(0, 0).astype(BF16)
                xcopy(0).start()
                sx[1] = total(0, 1).astype(BF16)
                xcopy(1).start()
            elif i == 1:
                sx[2] = total(1, 0).astype(BF16)
                xcopy(2).start()
            elif i == 2:
                sx[4] = total(2, 1).astype(BF16)
                xcopy(4).start()

        def relay():
            xcopy(1).wait_recv()
            sx[3] = (total(1, 1) + rx[1].astype(F32)).astype(BF16)
            xcopy(3).start()
            xcopy(0).wait_recv()
            sx[5] = (total(2, 0) + rx[0].astype(F32)).astype(BF16)
            xcopy(5).start()

        def result():
            for j in (2, 4, 3, 5):
                xcopy(j).wait_recv()
            low = total(3, 0) + rx[2].astype(F32) + rx[5].astype(F32)
            high = total(3, 1) + rx[4].astype(F32) + rx[3].astype(F32)
            return low, high

        def finish():
            for i in range(4):
                to_sib(i).wait_send()
            for j in range(6):
                xcopy(j).wait_send()

        return to_sib, stage, relay, result, finish

    def kv_copy():
        return remote(
            kvx.at[:, :, pl.ds(512, 128)],
            kvx.at[:, :, pl.ds(0, 128)],
            kv_sem.at[0],
            kv_sem.at[1],
            nxt,
        )

    kv_copy().start()
    wsteps[0]()
    kv_copy().wait_recv()

    to_sib, stage, relay, result, rfinish = reducer(
        p_own, p_sib, r_sib, s_x, r_x, a_ss, a_rs, ax_ss, ax_rs
    )

    def attend(i):
        n = (x + order[i]) % 4
        row = lax.broadcasted_iota(jnp.int32, (WINDOW, 2 * WINDOW), 0)
        col = lax.broadcasted_iota(jnp.int32, (WINDOW, 2 * WINDOW), 1)
        start = jnp.where((n == 0) & (sp == 0), WINDOW, 0)
        seen = (col > row) & (col <= row + WINDOW) & (col >= start)
        off = pl.multiple_of(n * WINDOW, WINDOW)
        kt = kvx[0, :, pl.ds(off, 2 * WINDOW)]
        vt = kvx[1, :, pl.ds(off, 2 * WINDOW)]
        nil = jnp.zeros_like(kt)
        keys = (jnp.concatenate([kt, nil], axis=0), jnp.concatenate([nil, kt], axis=0))
        vals = (jnp.concatenate([vt, nil], axis=0), jnp.concatenate([nil, vt], axis=0))
        for g in range(2):
            q2 = q_ref[pl.ds(off, WINDOW), 128 * g : 128 * g + 128]
            acc = jnp.zeros((WINDOW, 128), F32)
            for e in range(2):
                sink = sink_ref[2 * g + e]
                scores = jnp.dot(q2, keys[e], preferred_element_type=F32) * HD**-0.5
                scores = jnp.where(seen, scores, NEG_FILL)
                top = jnp.maximum(jnp.max(scores, axis=-1, keepdims=True), sink)
                expo = jnp.exp(scores - top)
                total = jnp.sum(expo, axis=-1, keepdims=True) + jnp.exp(sink - top)
                probs = (expo / total).astype(BF16)
                acc = acc + lax.dot_general(probs, vals[e], NT, preferred_element_type=F32)
            att[:, 128 * g : 128 * g + 128] = acc.astype(BF16)
        for j in range(4):
            cols = slice(512 * j, 512 * j + 512)
            for half, dst in ((1 - c, p_sib), (c, p_own)):
                part = att[pl.ds(pl.multiple_of(64 * half, 64), 64), :]
                dst[i, :, cols] = jnp.dot(
                    part, ow_ref[:, cols], preferred_element_type=F32
                ).astype(BF16)
        to_sib(i).start()

    attend(0)
    wsteps[1]()
    attend(1)
    stage(0)
    wsteps[2]()
    attend(2)
    stage(1)
    wsteps[3]()
    attend(3)
    stage(2)
    wsteps[4]()
    relay()
    stage(3)
    wsteps[5]()

    halves = result()
    for h in range(2):
        rows = slice(32 * h, 32 * h + 32)
        middle = res_ref[rows, :].astype(F32) + rms_scale(halves[h]) * ga_ref[...]
        mid[rows, :] = middle
        x_all[tp, h] = (rms_scale(middle) * gb_ref[...]).astype(BF16)

    tpm, tpp, tp2 = tp_at(x + 3, c), tp_at(x + 1, c), tp_at(x + 2, c)

    def gcopy(j):
        idx, half, dev = (
            (tp, 0, xp), (tp, 1, xm), (tp, 1, xp), (tp, 0, xm), (tpm, 0, xp), (tpp, 1, xm),
            (tpm, 0, sib), (tpp, 1, sib), (tpm, 1, sib), (tpp, 0, sib), (tp2, 0, sib), (tp2, 1, sib),
        )[j]
        ref = x_all.at[idx, half]
        return remote(ref, ref, g_ss.at[j], g_rs.at[j], dev)

    def gown():
        ref = x_all.at[tp]
        return remote(ref, ref, g_ss.at[12], g_rs.at[12], sib)

    for j in range(4):
        gcopy(j).start()
    gown().start()
    wsteps[6]()
    gcopy(0).wait_recv()
    gcopy(4).start()
    gcopy(6).start()
    gcopy(1).wait_recv()
    gcopy(5).start()
    gcopy(7).start()
    wsteps[7]()
    gcopy(2).wait_recv()
    gcopy(8).start()
    gcopy(3).wait_recv()
    gcopy(9).start()
    wsteps[8]()
    dsteps[0]()
    gcopy(4).wait_recv()
    gcopy(10).start()
    gcopy(5).wait_recv()
    gcopy(11).start()
    for j in range(6, 12):
        gcopy(j).wait_recv()
    gown().wait_recv()
    wsteps[9]()
    dsteps[1]()
    wsteps[10]()
    dsteps[2]()
    wsteps[11]()
    dsteps[3]()

    def up_copy(k):
        return remote(
            up.at[k, pl.ds(512, 8), :], up.at[k, pl.ds(0, 8), :], up_ss.at[k], up_rs.at[k], nxt
        )

    def project(k):
        width = 256 if k < 5 else 128
        cols = slice(256 * k, 256 * k + width)
        for m in range(2):
            left = x_all[4 * m : 4 * m + 4].reshape(256, 2048)
            right = gv[:, :, :, :, cols].reshape(2048, width)
            made = jnp.dot(left, right, preferred_element_type=F32)
            up[k, 8 + 256 * m : 264 + 256 * m, 0:width] = made.astype(BF16).astype(F32)
        up_copy(k).start()

    def conv(k, lanes, taps):
        total = taps[0:1] * up[k, 6:518, lanes]
        total = total + taps[1:2] * up[k, 7:519, lanes]
        return total + taps[2:3] * up[k, 8:520, lanes]

    def silu(v):
        return v / (1.0 + jnp.exp(-v))

    def gate(k):
        up_copy(k).wait_recv()
        up[k, 0:8, :] = jnp.where(sp > 0, up[k, 0:8, :], 0.0)
        if k < 5:
            cols = slice(128 * k, 128 * k + 128)
            made = silu(conv(k, slice(0, 128), gt_ref[:, cols])) * conv(
                k, slice(128, 256), vt2_ref[:, cols]
            )
        else:
            cols = slice(640, 768)
            taps = jnp.concatenate([gt_ref[:, 640:704], vt2_ref[:, 640:704]], axis=1)
            both = conv(k, slice(0, 128), taps)
            lane = lax.broadcasted_iota(jnp.int32, both.shape, 1)
            made = jnp.where(lane < 64, silu(both) * pltpu.roll(both, 64, 1), 0.0)
        hid[:, :, cols] = made.astype(BF16).reshape(8, 64, 128)

    project(0)
    project(1)
    dsteps[4]()
    project(2)
    project(3)
    dsteps[5]()
    project(4)
    project(5)
    dsteps[6]()
    gate(0)
    gate(1)
    gate(2)
    dsteps[7]()
    gate(3)
    gate(4)
    gate(5)
    for s in dsteps[8:]:
        s()

    to_sib2, stage2, relay2, result2, rfinish2 = reducer(
        f_own, f_sib, g_sib, t_x, u_x, b_ss, b_rs, bx_ss, bx_rs
    )
    for i in range(4):
        n = (x + order[i]) % 4
        for half, dst in ((1 - c, f_sib), (c, f_own)):
            left = hid[2 * n + half]
            for j in range(4):
                right = dn[2 * j : 2 * j + 2].reshape(512, 768)
                dst[i, :, 512 * j : 512 * j + 512] = lax.dot_general(
                    left, right, NT, preferred_element_type=F32
                ).astype(BF16)
        to_sib2(i).start()
        if i > 0:
            stage2(i - 1)
    relay2()
    stage2(3)
    halves = result2()
    for h in range(2):
        rows = slice(32 * h, 32 * h + 32)
        out_ref[rows, :] = (mid[rows, :] + rms_scale(halves[h]) * gc_ref[...]).astype(BF16)

    kv_copy().wait_send()
    for k in range(6):
        up_copy(k).wait_send()
    for j in range(12):
        gcopy(j).wait_send()
    gown().wait_send()
    rfinish()
    rfinish2()
    wfinish()
    dfinish()


def on_device(
    queries, key_states, value_states, sink_logits, out_weight, residual,
    gain_attn, gain_before, gain_after, gate_weight, value_weight, gate_taps, value_taps, down_weight,
):
    dma = pltpu.SemaphoreType.DMA
    vmem = pl.BlockSpec(memory_space=pltpu.VMEM)
    specs = [vmem] * 14
    specs[3] = pl.BlockSpec(memory_space=pltpu.SMEM)
    reduce_bufs = [
        pltpu.VMEM((4, 64, 2048), BF16),
        pltpu.VMEM((4, 64, 2048), BF16),
        pltpu.VMEM((4, 64, 2048), BF16),
        pltpu.VMEM((6, 32, 2048), BF16),
        pltpu.VMEM((6, 32, 2048), BF16),
    ]
    return pl.pallas_call(
        kernel,
        out_shape=jax.ShapeDtypeStruct((64, 2048), BF16),
        in_specs=specs,
        out_specs=vmem,
        scratch_shapes=[
            pltpu.VMEM((8, 8, 2, 16, 1408), BF16),
            pltpu.VMEM((8, 8, 2, 16, 768), BF16),
            pltpu.VMEM((2, 64, 640), BF16),
            pltpu.VMEM((128, 256), BF16),
            pltpu.VMEM((8, 2, 32, 2048), BF16),
            pltpu.VMEM((6, 520, 256), F32),
            pltpu.VMEM((8, 64, 768), BF16),
            pltpu.VMEM((64, 2048), F32),
            *reduce_bufs,
            *reduce_bufs,
            dma((2, 2, 2, 4)),
            dma((2, 2, 2, 4, 2)),
            dma((2, 2, 2, 5)),
            dma((2,)),
            dma((6,)),
            dma((6,)),
            dma((4,)),
            dma((4,)),
            dma((6,)),
            dma((6,)),
            dma((4,)),
            dma((4,)),
            dma((6,)),
            dma((6,)),
            dma((13,)),
            dma((13,)),
        ],
        compiler_params=pltpu.CompilerParams(
            collective_id=0, has_side_effects=True, vmem_limit_bytes=58 * 1024 * 1024
        ),
    )(
        queries, key_states.T, value_states.T, sink_logits, out_weight, residual,
        gain_attn.reshape(1, -1), gain_before.reshape(1, -1), gain_after.reshape(1, -1),
        gate_weight, value_weight, gate_taps, value_taps, down_weight.T,
    )


def solution(mesh):
    in_specs = (
        P("sp", "tp"), P("sp", "tp"), P("sp", "tp"), P("tp"), P("tp", None), P(("sp", "tp"), None),
        P(), P(), P(), P("sp", "tp"), P("sp", "tp"), P(None, "tp"), P(None, "tp"), P("tp", "sp"),
    )
    return jax.shard_map(
        on_device, mesh=mesh, in_specs=in_specs, out_specs=P(("sp", "tp"), None), check_vma=False
    )
```

```python
import jax
import jax.numpy as jnp
from jax import lax
from jax.experimental import pallas as pl
from jax.experimental.pallas import tpu as pltpu
from jax.sharding import PartitionSpec as P

HD = 64
WINDOW = 128
NEG_FILL = -1e30
MESH = pl.DeviceIdType.MESH
F32 = jnp.float32
BF16 = jnp.bfloat16
NT = (((1,), (1,)), ((), ()))


def rms_scale(matrix):
    return matrix * lax.rsqrt(jnp.mean(matrix * matrix, axis=-1, keepdims=True) + 1e-06)


def kernel(
    q_ref, kt_ref, vt_ref, sink_ref, ow_ref, res_ref, ga_ref, gb_ref, gc_ref,
    gw_ref, vw_ref, gt_ref, vt2_ref, dw_ref,
    out_ref,
    gv, dn, kvx, att, x_all, up, hid, mid,
    p_own, p_sib, r_sib, s_x, r_x,
    f_own, f_sib, g_sib, t_x, u_x, t_r, u_r, nat, squares,
    wp1, wp2, w_ss, dp1, dp2, d_ss, kv_sem, up_ss, up_rs,
    a_ss, a_rs, ax_ss, ax_rs, g_ss, g_rs, b_ss, b_rs,
):
    sp = lax.axis_index("sp")
    tp = lax.axis_index("tp")
    z, y = sp // 8, sp % 8
    x, c = tp // 2, tp % 2

    def at(zz, yy):
        return (zz % 8) * 8 + yy % 8

    def tp_at(xx, cc):
        return (xx % 4) * 2 + cc

    nxt, prv = ((sp + 1) % 64, tp), ((sp + 63) % 64, tp)
    sib = (sp, tp_at(x, 1 - c))
    xp, xm = (sp, tp_at(x + 1, c)), (sp, tp_at(x + 3, c))
    zn = ((at(z + 1, y), tp), (at(z + 7, y), tp))
    yn = ((at(z, y + 1), tp), (at(z, y + 7), tp))

    barrier = pltpu.get_barrier_semaphore()
    for dev in (nxt, prv, sib, xp, xm, *zn, *yn):
        pl.semaphore_signal(barrier, inc=1, device_id=dev, device_id_type=MESH)

    def remote(src, dst, ss, rs, dev):
        return pltpu.make_async_remote_copy(
            src_ref=src, dst_ref=dst, send_sem=ss, recv_sem=rs, device_id=dev, device_id_type=MESH
        )

    for h in range(2):
        rows = slice(16 * h, 16 * h + 16)
        for k in range(5):
            cols = slice(128 * k, 128 * k + 128)
            gv[z, y, h, :, 256 * k : 256 * k + 128] = gw_ref[rows, cols]
            gv[z, y, h, :, 256 * k + 128 : 256 * k + 256] = vw_ref[rows, cols]
            dn[z, y, h, :, cols] = dw_ref[rows, cols]
        gv[z, y, h, :, 1280:1408] = jnp.concatenate(
            [gw_ref[rows, 640:704].astype(F32), vw_ref[rows, 640:704].astype(F32)], axis=1
        ).astype(BF16)
        dn[z, y, h, :, 640:768] = jnp.concatenate(
            [dw_ref[rows, 640:704].astype(F32), jnp.zeros((16, 64), F32)], axis=1
        ).astype(BF16)
    kvx[0, :, 128:640] = kt_ref[...]
    kvx[1, :, 128:640] = vt_ref[...]

    pl.semaphore_wait(barrier, 9)

    def gather_steps(buf, rp1, rp2, ssem, size):
        count = 8 // size
        first = (y, z)
        second = (z, y)
        fdev = (yn, zn)
        sdev = (zn, yn)

        def item(h, f, s):
            f, s = f % 8, s % 8
            return buf.at[s, f, 0] if h == 0 else buf.at[f, s, 1]

        def batch(h, b, s):
            s = s % 8
            part = pl.ds(size * b, size)
            return buf.at[s, part, 0] if h == 0 else buf.at[part, s, 1]

        def hop(h, d, k):
            return first[h] + 8 - k if d == 0 else first[h] + k

        def group(h, d, k):
            return second[h] + 8 - k if d == 0 else second[h] + k

        def send_first(h, d, k):
            ref = item(h, hop(h, d, k - 1), second[h])
            remote(ref, ref, ssem.at[h, d, 0], rp1.at[h, d, k - 1], fdev[h][d]).start()

        def wait_first(h, d, k):
            ref = item(h, hop(h, d, k), second[h])
            remote(ref, ref, ssem.at[h, d, 0], rp1.at[h, d, k - 1], fdev[h][d]).wait_recv()

        def send_item(h, f):
            f = f % 8
            ref = item(h, f, second[h])
            for d in range(2):
                remote(ref, ref, ssem.at[h, d, 1], rp2.at[h, d, 0, f // size], sdev[h][d]).start()

        def wait_second(h, d, k, b):
            ref = batch(h, b, group(h, d, k))
            remote(ref, ref, ssem.at[h, d, 1], rp2.at[h, d, k - 1, b], sdev[h][d]).wait_recv()

        def forward(h, d, k, b):
            ref = batch(h, b, group(h, d, k))
            remote(ref, ref, ssem.at[h, d, k + 1], rp2.at[h, d, k, b], sdev[h][d]).start()

        def step_own(items):
            for h in range(2):
                for d in range(2):
                    send_first(h, d, 1)
            if items:
                for h in range(2):
                    send_item(h, first[h])

        def step_first(k, items):
            for d in range(2 if k < 4 else 1):
                for h in range(2):
                    wait_first(h, d, k)
                    if k < 4 - d:
                        send_first(h, d, k + 1)
                    if items:
                        send_item(h, hop(h, d, k))

        def step_group():
            for b in range(count):
                for h in range(2):
                    for d in range(2):
                        forward(h, d, 0, b)

        def step_second(k, b):
            for h in range(2):
                for d in range(2):
                    wait_second(h, d, k, b)
                    if k < 3 or b // (count // 2) == d:
                        forward(h, d, k, b)

        def step_last(b):
            for h in range(2):
                for d in range(2):
                    wait_second(h, d, 4, d * (count // 2) + b)

        def finish():
            for h in range(2):
                for d in range(2):
                    for slot, ref in (
                        (0, buf.at[0, pl.ds(0, 4 - d), 0]),
                        (1, buf.at[0, :, 0]),
                        (2, buf.at[0, :, 0]),
                        (3, buf.at[0, :, 0]),
                        (4, buf.at[0, pl.ds(0, 4), 0]),
                    ):
                        remote(ref, ref, ssem.at[h, d, slot], rp1.at[h, d, 0], sib).wait_send()

        return step_own, step_first, step_group, step_second, step_last, finish

    w_own, w_first, _, w_second, w_last, w_finish = gather_steps(gv, wp1, wp2, w_ss, 4)
    d_own, d_first, d_group, d_second, d_last, d_finish = gather_steps(dn, dp1, dp2, d_ss, 2)

    order = (2, 1, 3, 0)

    def reducer(own, sendb, recvb, sx, rx, ss, rs, xss, xrs):
        dest = (xm, xp, xp, xp, xm, xm)

        def xcopy(j):
            return remote(sx.at[j], rx.at[j], xss.at[j], xrs.at[j], dest[j])

        def to_sib(i):
            return remote(sendb.at[i], recvb.at[i], ss.at[i], rs.at[i], sib)

        def total(i, half):
            rows = slice(32 * half, 32 * half + 32)
            return own[i, rows].astype(F32) + recvb[i, rows].astype(F32)

        def stage(i):
            to_sib(i).wait_recv()
            if i == 0:
                sx[0] = total(0, 0).astype(BF16)
                xcopy(0).start()
                sx[1] = total(0, 1).astype(BF16)
                xcopy(1).start()
            elif i == 1:
                sx[2] = total(1, 0).astype(BF16)
                xcopy(2).start()
            elif i == 2:
                sx[4] = total(2, 1).astype(BF16)
                xcopy(4).start()

        def relay():
            xcopy(1).wait_recv()
            sx[3] = (total(1, 1) + rx[1].astype(F32)).astype(BF16)
            xcopy(3).start()
            xcopy(0).wait_recv()
            sx[5] = (total(2, 0) + rx[0].astype(F32)).astype(BF16)
            xcopy(5).start()

        def result():
            for j in (2, 4, 3, 5):
                xcopy(j).wait_recv()
            low = total(3, 0) + rx[2].astype(F32) + rx[5].astype(F32)
            high = total(3, 1) + rx[4].astype(F32) + rx[3].astype(F32)
            return low, high

        def finish():
            for i in range(4):
                to_sib(i).wait_send()
            for j in range(6):
                xcopy(j).wait_send()

        return to_sib, stage, relay, result, finish

    def kv_copy():
        return remote(
            kvx.at[:, :, pl.ds(512, 128)],
            kvx.at[:, :, pl.ds(0, 128)],
            kv_sem.at[0],
            kv_sem.at[1],
            nxt,
        )

    to_sib, stage, relay, result, rfinish = reducer(
        p_own, p_sib, r_sib, s_x, r_x, a_ss, a_rs, ax_ss, ax_rs
    )

    def attend(i):
        n = (x + order[i]) % 4
        row = lax.broadcasted_iota(jnp.int32, (WINDOW, 2 * WINDOW), 0)
        col = lax.broadcasted_iota(jnp.int32, (WINDOW, 2 * WINDOW), 1)
        start = jnp.where((n == 0) & (sp == 0), WINDOW, 0)
        seen = (col > row) & (col <= row + WINDOW) & (col >= start)
        off = pl.multiple_of(n * WINDOW, WINDOW)
        kt = kvx[0, :, pl.ds(off, 2 * WINDOW)]
        vt = kvx[1, :, pl.ds(off, 2 * WINDOW)]
        nil = jnp.zeros_like(kt)
        keys = (jnp.concatenate([kt, nil], axis=0), jnp.concatenate([nil, kt], axis=0))
        vals = (jnp.concatenate([vt, nil], axis=0), jnp.concatenate([nil, vt], axis=0))
        for g in range(2):
            q2 = q_ref[pl.ds(off, WINDOW), 128 * g : 128 * g + 128]
            acc = jnp.zeros((WINDOW, 128), F32)
            for e in range(2):
                sink = sink_ref[2 * g + e]
                scores = jnp.dot(q2, keys[e], preferred_element_type=F32) * HD**-0.5
                scores = jnp.where(seen, scores, NEG_FILL)
                top = jnp.maximum(jnp.max(scores, axis=-1, keepdims=True), sink)
                expo = jnp.exp(scores - top)
                total = jnp.sum(expo, axis=-1, keepdims=True) + jnp.exp(sink - top)
                probs = (expo / total).astype(BF16)
                acc = acc + lax.dot_general(probs, vals[e], NT, preferred_element_type=F32)
            att[:, 128 * g : 128 * g + 128] = acc.astype(BF16)
        for j in range(4):
            cols = slice(512 * j, 512 * j + 512)
            for half, dst in ((1 - c, p_sib), (c, p_own)):
                part = att[pl.ds(pl.multiple_of(64 * half, 64), 64), :]
                dst[i, :, cols] = jnp.dot(
                    part, ow_ref[:, cols], preferred_element_type=F32
                ).astype(BF16)
        to_sib(i).start()

    def norms():
        halves = result()
        for h in range(2):
            rows = slice(32 * h, 32 * h + 32)
            middle = res_ref[rows, :].astype(F32) + rms_scale(halves[h]) * ga_ref[...]
            mid[rows, :] = middle
            x_all[tp, h] = (rms_scale(middle) * gb_ref[...]).astype(BF16)
        for j in range(4):
            gcopy(j).start()
        gown().start()

    tpm, tpp, tp2 = tp_at(x + 3, c), tp_at(x + 1, c), tp_at(x + 2, c)

    def gcopy(j):
        idx, half, dev = (
            (tp, 0, xp), (tp, 1, xm), (tp, 1, xp), (tp, 0, xm), (tpm, 0, xp), (tpp, 1, xm),
            (tpm, 0, sib), (tpp, 1, sib), (tpm, 1, sib), (tpp, 0, sib), (tp2, 0, sib), (tp2, 1, sib),
        )[j]
        ref = x_all.at[idx, half]
        return remote(ref, ref, g_ss.at[j], g_rs.at[j], dev)

    def gown():
        ref = x_all.at[tp]
        return remote(ref, ref, g_ss.at[12], g_rs.at[12], sib)

    def pass_on(j, *after):
        gcopy(j).wait_recv()
        for k in after:
            gcopy(k).start()

    def rows_in():
        for j in range(6, 12):
            gcopy(j).wait_recv()
        gown().wait_recv()

    def up_copy(k):
        return remote(
            up.at[k, pl.ds(512, 8), :], up.at[k, pl.ds(0, 8), :], up_ss.at[k], up_rs.at[k], nxt
        )

    def project(k):
        width = 256 if k < 5 else 128
        cols = slice(256 * k, 256 * k + width)
        for m in range(2):
            left = x_all[4 * m : 4 * m + 4].reshape(256, 2048)
            right = gv[:, :, :, :, cols].reshape(2048, width)
            made = jnp.dot(left, right, preferred_element_type=F32)
            up[k, 8 + 256 * m : 264 + 256 * m, 0:width] = made.astype(BF16).astype(F32)
        up_copy(k).start()

    def conv(k, lanes, taps):
        total = taps[0:1] * up[k, 6:518, lanes]
        total = total + taps[1:2] * up[k, 7:519, lanes]
        return total + taps[2:3] * up[k, 8:520, lanes]

    def silu(v):
        return v / (1.0 + jnp.exp(-v))

    def gate(k):
        up_copy(k).wait_recv()
        up[k, 0:8, :] = jnp.where(sp > 0, up[k, 0:8, :], 0.0)
        if k < 5:
            cols = slice(128 * k, 128 * k + 128)
            made = silu(conv(k, slice(0, 128), gt_ref[:, cols])) * conv(
                k, slice(128, 256), vt2_ref[:, cols]
            )
        else:
            cols = slice(640, 768)
            taps = jnp.concatenate([gt_ref[:, 640:704], vt2_ref[:, 640:704]], axis=1)
            both = conv(k, slice(0, 128), taps)
            lane = lax.broadcasted_iota(jnp.int32, both.shape, 1)
            made = jnp.where(lane < 64, silu(both) * pltpu.roll(both, 64, 1), 0.0)
        made = made.astype(BF16)
        for b in range(8):
            slot = (b // 2 + 4 - x) % 4 + 4 * (1 - (c + b) % 2)
            hid[slot, :, cols] = made[64 * b : 64 * b + 64]

    def groups(k):
        if k in (0, 4):
            return [(0, z + k), (1, y + k)]
        return [(0, z + 8 - k), (0, z + k), (1, y + 8 - k), (1, y + k)]

    edges = (0, 256, 768, 1280, 1792, 2048)

    def span(k):
        return pl.ds(edges[k], edges[k + 1] - edges[k])

    def sib_copy(k):
        return remote(
            f_sib.at[:, :, span(k)], g_sib.at[:, :, span(k)], b_ss.at[0, k], b_rs.at[0, k], sib
        )

    def x_copy(k, d):
        return remote(
            t_x.at[d, :, :, span(k)], u_x.at[d, :, :, span(k)],
            b_ss.at[1 + d, k], b_rs.at[1 + d, k], (xp, xm)[d],
        )

    def r_copy(k, d):
        return remote(
            t_r.at[d, :, span(k)], u_r.at[d, :, span(k)],
            b_ss.at[3 + d, k], b_rs.at[3 + d, k], (xp, xm)[d],
        )

    def down(k):
        right = [
            (dn[g % 8, :, 0] if h == 0 else dn[:, g % 8, 1]).reshape(128, 768)
            for h, g in groups(k)
        ]
        made = lax.dot_general(
            hid[...].reshape(512, 768), jnp.concatenate(right, axis=0), NT,
            preferred_element_type=F32,
        ).astype(BF16).reshape(8, 64, 128 * len(right))
        f_sib[:, :, span(k)] = made[0:4]
        f_own[:, :, span(k)] = made[4:8]
        sib_copy(k).start()

    def both(k, i, half):
        rows = slice(32 * half, 32 * half + 32)
        return f_own[i, rows, span(k)].astype(F32) + g_sib[i, rows, span(k)].astype(F32)

    def spread(k):
        sib_copy(k).wait_recv()
        t_x[0, 0, :, span(k)] = both(k, 2, 1).astype(BF16)
        t_x[0, 1, :, span(k)] = both(k, 1, 0).astype(BF16)
        x_copy(k, 0).start()
        t_x[1, 0, :, span(k)] = both(k, 2, 0).astype(BF16)
        t_x[1, 1, :, span(k)] = both(k, 3, 1).astype(BF16)
        x_copy(k, 1).start()

    def relayed(k):
        x_copy(k, 0).wait_recv()
        t_r[0, :, span(k)] = (both(k, 1, 1) + u_x[0, 0, :, span(k)].astype(F32)).astype(BF16)
        r_copy(k, 0).start()
        x_copy(k, 1).wait_recv()
        t_r[1, :, span(k)] = (both(k, 3, 0) + u_x[1, 0, :, span(k)].astype(F32)).astype(BF16)
        r_copy(k, 1).start()

    def place(k):
        lane = lax.broadcasted_iota(jnp.int32, (32, 128), 1) // 16
        for half in range(2):
            rows = slice(32 * half, 32 * half + 32)
            r_copy(k, 1 - half).wait_recv()
            total = both(k, 0, half) + u_x[half, 1, :, span(k)].astype(F32)
            total = total + u_r[1 - half, :, span(k)].astype(F32)
            for j, (h, g) in enumerate(groups(k)):
                g = g % 8
                piece = total[:, 128 * j : 128 * j + 128]
                if k == 0 and j == 0:
                    squares[rows, :] = piece * piece
                else:
                    squares[rows, :] += piece * piece
                for t in range(8):
                    if h == 0:
                        where, shift, spot = (g, t // 4), 16 * t, 2 * (t % 4)
                    else:
                        where, spot = (t, g // 4), 2 * (g % 4) + 1
                        shift = (16 * spot + 128 - 16 * t) % 128
                    moved = pltpu.roll(piece, shift, 1)
                    nat[where[0], where[1], rows, :] = jnp.where(
                        lane == spot, moved, nat[where[0], where[1], rows, :]
                    )

    def last():
        scale = lax.rsqrt(jnp.sum(squares[...], axis=-1, keepdims=True) * (1.0 / 2048) + 1e-06)
        for j in range(16):
            cols = slice(128 * j, 128 * j + 128)
            out_ref[:, cols] = (
                mid[:, cols] + nat[j // 2, j % 2] * scale * gc_ref[:, cols]
            ).astype(BF16)

    def run(name, step, *args):
        with jax.named_scope(name):
            step(*args)

    run("kv_start", lambda: kv_copy().start())
    run("w0", w_own, True)
    run("kv_wait", lambda: kv_copy().wait_recv())
    for i in range(4):
        run(f"attend{i}", attend, i)
        if i > 0:
            run(f"stage{i - 1}", stage, i - 1)
        run(f"w{i + 1}", w_first, i + 1, True)
    run("relay", relay)
    run("stage3", stage, 3)
    run("w5", w_second, 1, 0)
    run("d_own", d_own, False)
    run("norms", norms)
    run("w6", w_second, 1, 1)
    run("d_f1", d_first, 1, False)
    run("pass0", pass_on, 0, 4, 6)
    run("pass1", pass_on, 1, 5, 7)
    run("w7", w_second, 2, 0)
    run("d_f2", d_first, 2, False)
    run("pass2", pass_on, 2, 8)
    run("pass3", pass_on, 3, 9)
    run("w8", w_second, 2, 1)
    run("d_f3", d_first, 3, False)
    run("pass4", pass_on, 4, 10)
    run("pass5", pass_on, 5, 11)
    run("rows_in", rows_in)
    run("w9", w_second, 3, 0)
    run("d_f4", d_first, 4, False)
    run("w10", w_second, 3, 1)
    run("d_group", d_group)
    run("w11", w_last, 0)
    steps = [(d_second, k, b) for k in range(1, 4) for b in range(4)] + [(d_last, 0), (d_last, 1)]

    def e(j):
        run(f"e{j}", *steps[j])

    for k in range(6):
        run(f"project{k}", project, k)
        e(k)
    for k in range(6):
        run(f"gate{k}", gate, k)
        if k % 2:
            e(6 + k // 2)
    run("down0", down, 0)
    e(9)
    run("down1", down, 1)
    run("spread0", spread, 0)
    e(10)
    run("down2", down, 2)
    run("spread1", spread, 1)
    run("relayed0", relayed, 0)
    e(11)
    run("down3", down, 3)
    run("spread2", spread, 2)
    run("relayed1", relayed, 1)
    run("place0", place, 0)
    e(12)
    run("spread3", spread, 3)
    run("relayed2", relayed, 2)
    run("place1", place, 1)
    e(13)
    run("down4", down, 4)
    run("relayed3", relayed, 3)
    run("spread4", spread, 4)
    run("place2", place, 2)
    run("relayed4", relayed, 4)
    run("place3", place, 3)
    run("place4", place, 4)
    run("last", last)

    kv_copy().wait_send()
    for k in range(6):
        up_copy(k).wait_send()
    for j in range(12):
        gcopy(j).wait_send()
    gown().wait_send()
    rfinish()
    for k in range(5):
        sib_copy(k).wait_send()
        for d in range(2):
            x_copy(k, d).wait_send()
            r_copy(k, d).wait_send()
    w_finish()
    d_finish()


def on_device(
    queries, key_states, value_states, sink_logits, out_weight, residual,
    gain_attn, gain_before, gain_after, gate_weight, value_weight, gate_taps, value_taps, down_weight,
):
    dma = pltpu.SemaphoreType.DMA
    vmem = pl.BlockSpec(memory_space=pltpu.VMEM)
    specs = [vmem] * 14
    specs[3] = pl.BlockSpec(memory_space=pltpu.SMEM)
    reduce_bufs = [
        pltpu.VMEM((4, 64, 2048), BF16),
        pltpu.VMEM((4, 64, 2048), BF16),
        pltpu.VMEM((4, 64, 2048), BF16),
        pltpu.VMEM((6, 32, 2048), BF16),
        pltpu.VMEM((6, 32, 2048), BF16),
    ]
    return pl.pallas_call(
        kernel,
        out_shape=jax.ShapeDtypeStruct((64, 2048), BF16),
        in_specs=specs,
        out_specs=vmem,
        scratch_shapes=[
            pltpu.VMEM((8, 8, 2, 16, 1408), BF16),
            pltpu.VMEM((8, 8, 2, 16, 768), BF16),
            pltpu.VMEM((2, 64, 640), BF16),
            pltpu.VMEM((128, 256), BF16),
            pltpu.VMEM((8, 2, 32, 2048), BF16),
            pltpu.VMEM((6, 520, 256), F32),
            pltpu.VMEM((8, 64, 768), BF16),
            pltpu.VMEM((64, 2048), F32),
            *reduce_bufs,
            *reduce_bufs[:3],
            pltpu.VMEM((2, 2, 32, 2048), BF16),
            pltpu.VMEM((2, 2, 32, 2048), BF16),
            pltpu.VMEM((2, 32, 2048), BF16),
            pltpu.VMEM((2, 32, 2048), BF16),
            pltpu.VMEM((8, 2, 64, 128), F32),
            pltpu.VMEM((64, 128), F32),
            dma((2, 2, 4)),
            dma((2, 2, 4, 2)),
            dma((2, 2, 5)),
            dma((2, 2, 4)),
            dma((2, 2, 4, 4)),
            dma((2, 2, 5)),
            dma((2,)),
            dma((6,)),
            dma((6,)),
            dma((4,)),
            dma((4,)),
            dma((6,)),
            dma((6,)),
            dma((13,)),
            dma((13,)),
            dma((5, 5)),
            dma((5, 5)),
        ],
        compiler_params=pltpu.CompilerParams(
            collective_id=0, has_side_effects=True, vmem_limit_bytes=58 * 1024 * 1024
        ),
    )(
        queries, key_states.T, value_states.T, sink_logits, out_weight, residual,
        gain_attn.reshape(1, -1), gain_before.reshape(1, -1), gain_after.reshape(1, -1),
        gate_weight, value_weight, gate_taps, value_taps, down_weight.T,
    )


def solution(mesh):
    in_specs = (
        P("sp", "tp"), P("sp", "tp"), P("sp", "tp"), P("tp"), P("tp", None), P(("sp", "tp"), None),
        P(), P(), P(), P("sp", "tp"), P("sp", "tp"), P(None, "tp"), P(None, "tp"), P("tp", "sp"),
    )
    return jax.shard_map(
        on_device, mesh=mesh, in_specs=in_specs, out_specs=P(("sp", "tp"), None), check_vma=False
    )
```

```python
import jax
import jax.numpy as jnp
from jax import lax
from jax.experimental import pallas as pl
from jax.experimental.pallas import tpu as pltpu
from jax.sharding import PartitionSpec as P

HD = 64
WINDOW = 128
NEG_FILL = -1e30
MESH = pl.DeviceIdType.MESH
F32 = jnp.float32
BF16 = jnp.bfloat16
NT = (((1,), (1,)), ((), ()))


def rms_scale(matrix):
    return matrix * lax.rsqrt(jnp.mean(matrix * matrix, axis=-1, keepdims=True) + 1e-06)


def kernel(
    q_hbm, kt_hbm, vt_hbm, sink_ref, ow_hbm, res_hbm, ga_ref, gb_ref, gc_ref,
    gw_hbm, vw_hbm, gt_ref, vt2_ref, dw_hbm,
    out_ref,
    q_ref, ow_ref, res_ref, gw_ref, vw_ref, dw_ref, in_sem,
    gv, dn, kvx, att, x_all, up, hid, mid,
    p_own, p_sib, r_sib, s_x, r_x,
    f_own, f_sib, g_sib, t_x, u_x, t_r, u_r, nat, squares,
    wp1, wp2, w_ss, dp1, dp2, d_ss, kv_sem, up_ss, up_rs,
    a_ss, a_rs, ax_ss, ax_rs, g_ss, g_rs, b_ss, b_rs,
):
    sp = lax.axis_index("sp")
    tp = lax.axis_index("tp")
    z, y = sp // 8, sp % 8
    x, c = tp // 2, tp % 2

    def at(zz, yy):
        return (zz % 8) * 8 + yy % 8

    def tp_at(xx, cc):
        return (xx % 4) * 2 + cc

    nxt, prv = ((sp + 1) % 64, tp), ((sp + 63) % 64, tp)
    sib = (sp, tp_at(x, 1 - c))
    xp, xm = (sp, tp_at(x + 1, c)), (sp, tp_at(x + 3, c))
    zn = ((at(z + 1, y), tp), (at(z + 7, y), tp))
    yn = ((at(z, y + 1), tp), (at(z, y + 7), tp))

    barrier = pltpu.get_barrier_semaphore()
    for dev in (nxt, prv, sib, xp, xm, *zn, *yn):
        pl.semaphore_signal(barrier, inc=1, device_id=dev, device_id_type=MESH)

    loads = (
        (q_hbm, q_ref), (ow_hbm, ow_ref), (res_hbm, res_ref), (gw_hbm, gw_ref), (vw_hbm, vw_ref),
        (dw_hbm, dw_ref), (kt_hbm, kvx.at[0, :, pl.ds(128, 512)]), (vt_hbm, kvx.at[1, :, pl.ds(128, 512)]),
    )

    def load(j):
        return pltpu.make_async_copy(loads[j][0], loads[j][1], in_sem.at[j])

    def fetched(*which):
        for j in which:
            load(j).wait()

    for j in (3, 4, 5, 6, 7, 0, 1, 2):
        load(j).start()

    def remote(src, dst, ss, rs, dev):
        return pltpu.make_async_remote_copy(
            src_ref=src, dst_ref=dst, send_sem=ss, recv_sem=rs, device_id=dev, device_id_type=MESH
        )

    fetched(3, 4, 5, 6, 7)
    for h in range(2):
        rows = slice(16 * h, 16 * h + 16)
        for k in range(5):
            cols = slice(128 * k, 128 * k + 128)
            gv[z, y, h, :, 256 * k : 256 * k + 128] = gw_ref[rows, cols]
            gv[z, y, h, :, 256 * k + 128 : 256 * k + 256] = vw_ref[rows, cols]
            dn[z, y, h, :, cols] = dw_ref[rows, cols]
        gv[z, y, h, :, 1280:1408] = jnp.concatenate(
            [gw_ref[rows, 640:704].astype(F32), vw_ref[rows, 640:704].astype(F32)], axis=1
        ).astype(BF16)
        dn[z, y, h, :, 640:768] = jnp.concatenate(
            [dw_ref[rows, 640:704].astype(F32), jnp.zeros((16, 64), F32)], axis=1
        ).astype(BF16)
    pl.semaphore_wait(barrier, 9)

    def gather_steps(buf, rp1, rp2, ssem, size):
        count = 8 // size
        first = (y, z)
        second = (z, y)
        fdev = (yn, zn)
        sdev = (zn, yn)
        links = tuple((h, d) for h in range(2) for d in range(2))

        def item(h, f, s):
            f, s = f % 8, s % 8
            return buf.at[s, f, 0] if h == 0 else buf.at[f, s, 1]

        def batch(h, b, s):
            s = s % 8
            part = pl.ds(size * ((first[h] // size + b) % count), size)
            return buf.at[s, part, 0] if h == 0 else buf.at[part, s, 1]

        def hop(h, d, k):
            return first[h] + 8 - k if d == 0 else first[h] + k

        def group(h, d, k):
            return second[h] + 8 - k if d == 0 else second[h] + k

        def arrived(items, sem):
            ref = buf.at[0, pl.ds(0, items), 0]
            remote(ref, ref, ssem.at[0], sem, sib).wait_recv()

        def send_first(h, d, k):
            ref = item(h, hop(h, d, k - 1), second[h])
            remote(ref, ref, ssem.at[0], rp1.at[k - 1], fdev[h][d]).start()

        def send_item(h, f):
            f = f % 8
            ref = item(h, f, second[h])
            slot = (f // size + count - first[h] // size) % count
            for d in range(2):
                remote(ref, ref, ssem.at[1], rp2.at[0, slot], sdev[h][d]).start()

        def forward(h, d, k, b):
            ref = batch(h, b, group(h, d, k))
            slot = b if k < 3 else b // 2
            remote(ref, ref, ssem.at[1], rp2.at[k, slot], sdev[h][d]).start()

        def step_own(items):
            for h, d in links:
                send_first(h, d, 1)
            if items:
                for h in range(2):
                    send_item(h, first[h])

        def step_first(k, items):
            arrived(4 if k < 4 else 2, rp1.at[k - 1])
            for h, d in links:
                if k < 4 - d:
                    send_first(h, d, k + 1)
            if items:
                for h, d in links:
                    if k <= 4 - d:
                        send_item(h, hop(h, d, k))

        def step_group(b):
            for h, d in links:
                forward(h, d, 0, b)

        def step_second(k, b):
            arrived(4 * size, rp2.at[k - 1, b])
            for h, d in links:
                if k < 3 or (b in (1, 2)) == d:
                    forward(h, d, k, b)

        def step_last(b):
            arrived(4 * size, rp2.at[3, b])

        def finish():
            ref = buf.at[0, pl.ds(0, 7)]
            remote(ref, ref, ssem.at[0], rp1.at[0], sib).wait_send()
            ref = buf.at[pl.ds(0, 7)]
            remote(ref, ref, ssem.at[1], rp1.at[0], sib).wait_send()

        return step_own, step_first, step_group, step_second, step_last, finish

    w_own, w_first, _, w_second, w_last, w_finish = gather_steps(gv, wp1, wp2, w_ss, 2)
    d_own, d_first, d_group, d_second, d_last, d_finish = gather_steps(dn, dp1, dp2, d_ss, 2)

    order = (2, 1, 3, 0)

    def reducer(own, sendb, recvb, sx, rx, ss, rs, xss, xrs):
        dest = (xm, xp, xp, xp, xm, xm)

        def xcopy(j):
            return remote(sx.at[j], rx.at[j], xss.at[0], xrs.at[min(j, 2)], dest[j])

        def to_sib(i):
            return remote(sendb.at[i], recvb.at[i], ss.at[0], rs.at[i], sib)

        def total(i, half):
            rows = slice(32 * half, 32 * half + 32)
            return own[i, rows].astype(F32) + recvb[i, rows].astype(F32)

        def stage(i):
            to_sib(i).wait_recv()
            if i == 0:
                sx[0] = total(0, 0).astype(BF16)
                xcopy(0).start()
                sx[1] = total(0, 1).astype(BF16)
                xcopy(1).start()
            elif i == 1:
                sx[2] = total(1, 0).astype(BF16)
                xcopy(2).start()
            elif i == 2:
                sx[4] = total(2, 1).astype(BF16)
                xcopy(4).start()

        def relay():
            xcopy(1).wait_recv()
            sx[3] = (total(1, 1) + rx[1].astype(F32)).astype(BF16)
            xcopy(3).start()
            xcopy(0).wait_recv()
            sx[5] = (total(2, 0) + rx[0].astype(F32)).astype(BF16)
            xcopy(5).start()

        def result():
            ref = rx.at[pl.ds(2, 4)]
            remote(ref, ref, xss.at[0], xrs.at[2], xp).wait_recv()
            low = total(3, 0) + rx[2].astype(F32) + rx[5].astype(F32)
            high = total(3, 1) + rx[4].astype(F32) + rx[3].astype(F32)
            return low, high

        def finish():
            remote(sendb, recvb, ss.at[0], rs.at[0], sib).wait_send()
            remote(sx, rx, xss.at[0], xrs.at[0], xp).wait_send()

        return to_sib, stage, relay, result, finish

    def kv_copy():
        return remote(
            kvx.at[:, :, pl.ds(512, 128)],
            kvx.at[:, :, pl.ds(0, 128)],
            kv_sem.at[0],
            kv_sem.at[1],
            nxt,
        )

    to_sib, stage, relay, result, rfinish = reducer(
        p_own, p_sib, r_sib, s_x, r_x, a_ss, a_rs, ax_ss, ax_rs
    )

    def attend(i):
        n = (x + order[i]) % 4
        row = lax.broadcasted_iota(jnp.int32, (WINDOW, 2 * WINDOW), 0)
        col = lax.broadcasted_iota(jnp.int32, (WINDOW, 2 * WINDOW), 1)
        start = jnp.where((n == 0) & (sp == 0), WINDOW, 0)
        seen = (col > row) & (col <= row + WINDOW) & (col >= start)
        off = pl.multiple_of(n * WINDOW, WINDOW)
        kt = kvx[0, :, pl.ds(off, 2 * WINDOW)]
        vt = kvx[1, :, pl.ds(off, 2 * WINDOW)]
        nil = jnp.zeros_like(kt)
        keys = (jnp.concatenate([kt, nil], axis=0), jnp.concatenate([nil, kt], axis=0))
        vals = (jnp.concatenate([vt, nil], axis=0), jnp.concatenate([nil, vt], axis=0))
        for g in range(2):
            q2 = q_ref[pl.ds(off, WINDOW), 128 * g : 128 * g + 128]
            acc = jnp.zeros((WINDOW, 128), F32)
            for e in range(2):
                sink = sink_ref[2 * g + e]
                scores = jnp.dot(q2, keys[e], preferred_element_type=F32) * HD**-0.5
                scores = jnp.where(seen, scores, NEG_FILL)
                top = jnp.maximum(jnp.max(scores, axis=-1, keepdims=True), sink)
                expo = jnp.exp(scores - top)
                total = jnp.sum(expo, axis=-1, keepdims=True) + jnp.exp(sink - top)
                probs = (expo / total).astype(BF16)
                acc = acc + lax.dot_general(probs, vals[e], NT, preferred_element_type=F32)
            att[:, 128 * g : 128 * g + 128] = acc.astype(BF16)
        for j in range(4):
            cols = slice(512 * j, 512 * j + 512)
            for half, dst in ((1 - c, p_sib), (c, p_own)):
                part = att[pl.ds(pl.multiple_of(64 * half, 64), 64), :]
                dst[i, :, cols] = jnp.dot(
                    part, ow_ref[:, cols], preferred_element_type=F32
                ).astype(BF16)
        to_sib(i).start()

    def norms():
        halves = result()
        for h in range(2):
            rows = slice(32 * h, 32 * h + 32)
            middle = res_ref[rows, :].astype(F32) + rms_scale(halves[h]) * ga_ref[...]
            mid[rows, :] = middle
            x_all[tp, h] = (rms_scale(middle) * gb_ref[...]).astype(BF16)
        for j in range(4):
            gcopy(j).start()
        gown().start()

    tpm, tpp, tp2 = tp_at(x + 3, c), tp_at(x + 1, c), tp_at(x + 2, c)

    def gcopy(j):
        idx, half, dev = (
            (tp, 0, xp), (tp, 1, xm), (tp, 1, xp), (tp, 0, xm), (tpm, 0, xp), (tpp, 1, xm),
            (tpm, 0, sib), (tpp, 1, sib), (tpm, 1, sib), (tpp, 0, sib), (tp2, 0, sib), (tp2, 1, sib),
        )[j]
        ref = x_all.at[idx, half]
        return remote(ref, ref, g_ss.at[0], g_rs.at[min(j, 6)], dev)

    def gown():
        ref = x_all.at[tp]
        return remote(ref, ref, g_ss.at[0], g_rs.at[6], sib)

    def pass_on(j, *after):
        gcopy(j).wait_recv()
        for k in after:
            gcopy(k).start()

    def rows_in():
        ref = x_all.at[pl.ds(0, 4)]
        remote(ref, ref, g_ss.at[0], g_rs.at[6], sib).wait_recv()

    def up_copy(k):
        return remote(
            up.at[k, pl.ds(512, 8), :], up.at[k, pl.ds(0, 8), :], up_ss.at[0], up_rs.at[k], nxt
        )

    def project(k):
        width = 256 if k < 5 else 128
        cols = slice(256 * k, 256 * k + width)
        for m in range(2):
            left = x_all[4 * m : 4 * m + 4].reshape(256, 2048)
            right = gv[:, :, :, :, cols].reshape(2048, width)
            made = jnp.dot(left, right, preferred_element_type=F32)
            up[k, 8 + 256 * m : 264 + 256 * m, 0:width] = made.astype(BF16).astype(F32)
        up_copy(k).start()

    def conv(k, lanes, taps):
        total = taps[0:1] * up[k, 6:518, lanes]
        total = total + taps[1:2] * up[k, 7:519, lanes]
        return total + taps[2:3] * up[k, 8:520, lanes]

    def silu(v):
        return v / (1.0 + jnp.exp(-v))

    def gate(k):
        up_copy(k).wait_recv()
        up[k, 0:8, :] = jnp.where(sp > 0, up[k, 0:8, :], 0.0)
        if k < 5:
            cols = slice(128 * k, 128 * k + 128)
            made = silu(conv(k, slice(0, 128), gt_ref[:, cols])) * conv(
                k, slice(128, 256), vt2_ref[:, cols]
            )
        else:
            cols = slice(640, 768)
            taps = jnp.concatenate([gt_ref[:, 640:704], vt2_ref[:, 640:704]], axis=1)
            both = conv(k, slice(0, 128), taps)
            lane = lax.broadcasted_iota(jnp.int32, both.shape, 1)
            made = jnp.where(lane < 64, silu(both) * pltpu.roll(both, 64, 1), 0.0)
        made = made.astype(BF16)
        for b in range(8):
            slot = (b // 2 + 4 - x) % 4 + 4 * (1 - (c + b) % 2)
            hid[slot, :, cols] = made[64 * b : 64 * b + 64]

    def groups(k):
        if k == 3:
            return [(0, z + 4), (1, y + 4)]
        near = [(0, z + 7 - k), (0, z + k + 1), (1, y + 7 - k), (1, y + k + 1)]
        return near if k else [(0, z), (1, y)] + near

    edges = (0, 768, 1280, 1792, 2048)

    def span(k):
        return pl.ds(edges[k], edges[k + 1] - edges[k])

    def sib_copy(k):
        return remote(
            f_sib.at[:, :, span(k)], g_sib.at[:, :, span(k)], b_ss.at[0], b_rs.at[0, k], sib
        )

    def x_copy(k, d):
        return remote(
            t_x.at[d, :, :, span(k)], u_x.at[d, :, :, span(k)],
            b_ss.at[1], b_rs.at[1, k], (xp, xm)[d],
        )

    def r_copy(k, d):
        return remote(
            t_r.at[d, :, span(k)], u_r.at[d, :, span(k)],
            b_ss.at[2], b_rs.at[2, k], (xp, xm)[d],
        )

    def down(k):
        right = [
            (dn[g % 8, :, 0] if h == 0 else dn[:, g % 8, 1]).reshape(128, 768)
            for h, g in groups(k)
        ]
        made = lax.dot_general(
            hid[...].reshape(512, 768), jnp.concatenate(right, axis=0), NT,
            preferred_element_type=F32,
        ).astype(BF16).reshape(8, 64, 128 * len(right))
        f_sib[:, :, span(k)] = made[0:4]
        f_own[:, :, span(k)] = made[4:8]
        sib_copy(k).start()

    def both(k, i, half):
        rows = slice(32 * half, 32 * half + 32)
        return f_own[i, rows, span(k)].astype(F32) + g_sib[i, rows, span(k)].astype(F32)

    def spread(k):
        sib_copy(k).wait_recv()
        t_x[0, 0, :, span(k)] = both(k, 2, 1).astype(BF16)
        t_x[0, 1, :, span(k)] = both(k, 1, 0).astype(BF16)
        x_copy(k, 0).start()
        t_x[1, 0, :, span(k)] = both(k, 2, 0).astype(BF16)
        t_x[1, 1, :, span(k)] = both(k, 3, 1).astype(BF16)
        x_copy(k, 1).start()

    def relayed(k):
        ref = u_x.at[:, :, :, span(k)]
        remote(ref, ref, b_ss.at[1], b_rs.at[1, k], xp).wait_recv()
        t_r[0, :, span(k)] = (both(k, 1, 1) + u_x[0, 0, :, span(k)].astype(F32)).astype(BF16)
        r_copy(k, 0).start()
        t_r[1, :, span(k)] = (both(k, 3, 0) + u_x[1, 0, :, span(k)].astype(F32)).astype(BF16)
        r_copy(k, 1).start()

    def place(k):
        lane = lax.broadcasted_iota(jnp.int32, (32, 128), 1) // 16
        ref = u_r.at[:, :, span(k)]
        remote(ref, ref, b_ss.at[2], b_rs.at[2, k], xp).wait_recv()
        for half in range(2):
            rows = slice(32 * half, 32 * half + 32)
            total = both(k, 0, half) + u_x[half, 1, :, span(k)].astype(F32)
            total = total + u_r[1 - half, :, span(k)].astype(F32)
            for j, (h, g) in enumerate(groups(k)):
                g = g % 8
                piece = total[:, 128 * j : 128 * j + 128]
                if k == 0 and j == 0:
                    squares[rows, :] = piece * piece
                else:
                    squares[rows, :] += piece * piece
                for t in range(8):
                    if h == 0:
                        where, shift, spot = (g, t // 4), 16 * t, 2 * (t % 4)
                    else:
                        where, spot = (t, g // 4), 2 * (g % 4) + 1
                        shift = (16 * spot + 128 - 16 * t) % 128
                    moved = pltpu.roll(piece, shift, 1)
                    nat[where[0], where[1], rows, :] = jnp.where(
                        lane == spot, moved, nat[where[0], where[1], rows, :]
                    )

    def last():
        scale = lax.rsqrt(jnp.sum(squares[...], axis=-1, keepdims=True) * (1.0 / 2048) + 1e-06)
        for j in range(16):
            cols = slice(128 * j, 128 * j + 128)
            out_ref[:, cols] = (
                mid[:, cols] + nat[j // 2, j % 2] * scale * gc_ref[:, cols]
            ).astype(BF16)

    def run(name, step, *args):
        with jax.named_scope(name):
            step(*args)

    run("kv_start", lambda: kv_copy().start())
    run("w0", w_own, True)
    run("d0", d_own, False)
    run("kv_wait", lambda: kv_copy().wait_recv())
    run("in_wait", lambda: fetched(0, 1))
    def first(k):
        run(f"w{k}", w_first, k, True)
        run(f"d{k}", d_first, k, False)

    run("attend0", attend, 0)
    first(1)
    run("attend1", attend, 1)
    run("stage0", stage, 0)
    run("attend2", attend, 2)
    first(2)
    run("stage1", stage, 1)
    run("w1_0", w_second, 1, 0)
    run("attend3", attend, 3)
    run("stage2", stage, 2)
    first(3)
    run("relay", relay)
    run("stage3", stage, 3)
    first(4)
    for b in (1, 3, 2):
        run(f"w1_{b}", w_second, 1, b)
    run("in_wait2", lambda: fetched(2))
    run("norms", norms)
    run("w2_0", w_second, 2, 0)
    run("w2_1", w_second, 2, 1)
    run("pass0", pass_on, 0, 4, 6)
    run("pass1", pass_on, 1, 5, 7)
    run("w2_3", w_second, 2, 3)
    run("w2_2", w_second, 2, 2)
    run("pass2", pass_on, 2, 8)
    run("pass3", pass_on, 3, 9)
    run("w3_0", w_second, 3, 0)
    run("w3_1", w_second, 3, 1)
    run("pass4", pass_on, 4, 10)
    run("pass5", pass_on, 5, 11)
    run("w3_3", w_second, 3, 3)
    run("w3_2", w_second, 3, 2)
    for b in (0, 1, 3, 2):
        run(f"d_g{b}", d_group, b)
    run("rows_in", rows_in)
    run("w4_0", w_last, 0)
    run("w4_1", w_last, 1)
    steps = [(d_second, k, b) for k in range(1, 4) for b in (0, 1, 3, 2)] + [(d_last, 0), (d_last, 1)]
    phases = {"p": project, "g": gate, "down": down, "spread": spread, "relayed": relayed, "place": place}
    for name in (
        "e0", "p0", "e1", "p1", "e2", "p2", "e3", "p3", "p4", "e4", "p5", "e5",
        "g0", "g1", "e6", "g2", "g3", "e7", "g4", "g5",
        "down0", "e8", "down1", "e9", "e10", "spread0", "e11", "spread1", "down2",
        "e12", "e13", "relayed0", "spread2", "down3", "relayed1",
        "place0", "spread3", "relayed2", "place1", "relayed3", "place2", "place3",
    ):
        base = name.rstrip("0123456789")
        j = int(name[len(base) :])
        if base == "e":
            run(name, *steps[j])
        else:
            run(name, phases[base], j)
    run("last", last)

    def finish():
        kv_copy().wait_send()
        ref = up.at[:, pl.ds(0, 8), :]
        remote(ref, ref, up_ss.at[0], up_rs.at[0], nxt).wait_send()
        ref = x_all.at[pl.ds(0, 7)]
        remote(ref, ref, g_ss.at[0], g_rs.at[0], sib).wait_send()
        rfinish()
        remote(f_sib, g_sib, b_ss.at[0], b_rs.at[0, 0], sib).wait_send()
        remote(t_x, u_x, b_ss.at[1], b_rs.at[1, 0], xp).wait_send()
        remote(t_r, u_r, b_ss.at[2], b_rs.at[2, 0], xp).wait_send()
        w_finish()
        d_finish()

    run("finish", finish)


def on_device(
    queries, key_states, value_states, sink_logits, out_weight, residual,
    gain_attn, gain_before, gain_after, gate_weight, value_weight, gate_taps, value_taps, down_weight,
):
    dma = pltpu.SemaphoreType.DMA
    vmem = pl.BlockSpec(memory_space=pltpu.VMEM)
    specs = [vmem] * 14
    specs[3] = pl.BlockSpec(memory_space=pltpu.SMEM)
    for j in (0, 1, 2, 4, 5, 9, 10, 13):
        specs[j] = pl.BlockSpec(memory_space=pltpu.HBM)
    reduce_bufs = [
        pltpu.VMEM((4, 64, 2048), BF16),
        pltpu.VMEM((4, 64, 2048), BF16),
        pltpu.VMEM((4, 64, 2048), BF16),
        pltpu.VMEM((6, 32, 2048), BF16),
        pltpu.VMEM((6, 32, 2048), BF16),
    ]
    return pl.pallas_call(
        kernel,
        out_shape=jax.ShapeDtypeStruct((64, 2048), BF16),
        in_specs=specs,
        out_specs=vmem,
        scratch_shapes=[
            pltpu.VMEM((512, 256), BF16),
            pltpu.VMEM((256, 2048), BF16),
            pltpu.VMEM((64, 2048), BF16),
            pltpu.VMEM((32, 704), BF16),
            pltpu.VMEM((32, 704), BF16),
            pltpu.VMEM((32, 704), BF16),
            dma((8,)),
            pltpu.VMEM((8, 8, 2, 16, 1408), BF16),
            pltpu.VMEM((8, 8, 2, 16, 768), BF16),
            pltpu.VMEM((2, 64, 640), BF16),
            pltpu.VMEM((128, 256), BF16),
            pltpu.VMEM((8, 2, 32, 2048), BF16),
            pltpu.VMEM((6, 520, 256), F32),
            pltpu.VMEM((8, 64, 768), BF16),
            pltpu.VMEM((64, 2048), F32),
            *reduce_bufs,
            *reduce_bufs[:3],
            pltpu.VMEM((2, 2, 32, 2048), BF16),
            pltpu.VMEM((2, 2, 32, 2048), BF16),
            pltpu.VMEM((2, 32, 2048), BF16),
            pltpu.VMEM((2, 32, 2048), BF16),
            pltpu.VMEM((8, 2, 64, 128), F32),
            pltpu.VMEM((64, 128), F32),
            dma((4,)),
            dma((4, 4)),
            dma((2,)),
            dma((4,)),
            dma((4, 4)),
            dma((2,)),
            dma((2,)),
            dma((1,)),
            dma((6,)),
            dma((1,)),
            dma((4,)),
            dma((1,)),
            dma((3,)),
            dma((1,)),
            dma((7,)),
            dma((3,)),
            dma((3, 4)),
        ],
        compiler_params=pltpu.CompilerParams(
            collective_id=0, has_side_effects=True, vmem_limit_bytes=60 * 1024 * 1024
        ),
    )(
        queries, key_states.T, value_states.T, sink_logits, out_weight, residual,
        gain_attn.reshape(1, -1), gain_before.reshape(1, -1), gain_after.reshape(1, -1),
        gate_weight, value_weight, gate_taps, value_taps, down_weight.T,
    )


def solution(mesh):
    in_specs = (
        P("sp", "tp"), P("sp", "tp"), P("sp", "tp"), P("tp"), P("tp", None), P(("sp", "tp"), None),
        P(), P(), P(), P("sp", "tp"), P("sp", "tp"), P(None, "tp"), P(None, "tp"), P("tp", "sp"),
    )
    return jax.shard_map(
        on_device, mesh=mesh, in_specs=in_specs, out_specs=P(("sp", "tp"), None), check_vma=False
    )
```
